32 devices in a mesh: grp: 2 (over y), sp: 4 (over z), dp: 4 (over x, core).
Axes of the slice: x: 2, y: 2, z: 4, core: 2. Of those that a mesh axis runs over, the one named last changes fastest.
Arguments:
- activations: bfloat16 [8, 2048, 2048], P(('grp', 'dp'), 'sp'), parts along dimension 0, may hold values from -6 to 6
- value_weight: bfloat16 [2048, 1024], P('sp', 'dp'), may hold values from -0.125 to 0.125
- gate_weight: bfloat16 [2048, 1024], P('sp', 'dp'), may hold values from -0.125 to 0.125
- conv_taps: float32 [31, 1024], replicated, may hold values from -4 to 4
- conv_bias: float32 [1024], replicated, may hold values from -3 to 3
- norm_gain: float32 [1024], replicated, may hold values from 0.1 to 1.9
- norm_bias: float32 [1024], replicated, may hold values from -3 to 3
- out_weight: bfloat16 [1024, 2048], P('sp', 'dp'), may hold values from -0.1875 to 0.1875
Outputs:
- mixed_out: bfloat16 [8, 2048, 2048], P(('grp', 'dp'), 'sp'), parts along dimension 0
The draws below stay inside these ranges and needn't reach their ends.
There are 2 independent parts, one for each index of `grp`. The reference program is written for one: setup_inputs(seed, part) draws one part's arguments, and reference() takes and returns one part's arrays. A program takes and returns all parts, laid end to end along the dimension named above; an argument that names none is the same for every part. Nothing has to cross between parts.
All inputs are finite; a program needn't handle non-finite values.
Results may differ from the reference program's by a relative error of at most 0.013.
Values may be sent and summed in bfloat16 or wider, within the bound.
A program may use at most 64 MiB of HBM per device.

```python
import jax
import jax.numpy as jnp
from jax import lax

D = 2048
C = 1024
KW = 31
LEN = 2048
SEQS = 4


def draw_conv_taps(key, part):
    key_base = jax.random.fold_in(key, 11)
    key_level = jax.random.fold_in(key, 12)
    blocks = C // 16
    levels = jax.random.uniform(key_level, (blocks,), jnp.float32, -1.2, 1.2)
    scales = jnp.repeat(jnp.exp(levels), 16)
    base = jnp.clip(jax.random.normal(key_base, (KW, C), jnp.float32), -3.0, 3.0)
    return jnp.clip(base * scales[None, :] * KW ** (-0.5), -4.0, 4.0)


def level_of(own_key, dims, shards, low, top_value):
    def one(dim, parts):
        heights = jax.random.uniform(jax.random.fold_in(jax.random.fold_in(own_key, 6), dim), (parts,), jnp.float32, low / len(shards), top_value / len(shards))
        return jnp.repeat(jnp.exp(heights), dims[dim] // parts).reshape((-1,) + (1,) * (len(dims) - dim - 1))

    factor_of = one(*shards[0])
    for cut in shards[1:]:
        factor_of = factor_of * one(*cut)
    return factor_of


def centred(rng, extent, scale, bound, pieces=(), kind=jnp.bfloat16):
    factor_of = level_of(rng, extent, pieces, -0.22, 0.18) if pieces else 1.0
    array = jax.random.normal(rng, extent, jnp.float32) * scale * factor_of
    return jnp.minimum(jnp.maximum(array, -bound), bound).astype(kind)


def setup_inputs(seed: int = 0, part: int = 0) -> dict:
    keys = jax.random.split(jax.random.key(seed), 9)
    own_keys = jax.random.split(jax.random.fold_in(keys[8], part), 9)
    return {
        "activations": centred(own_keys[0], (SEQS, LEN, D), 1.0, 6.0, ((0, 4), (1, 4))),
        "value_weight": centred(keys[1], (D, C), D ** -0.5, 0.125, ((0, 4), (1, 4))),
        "gate_weight": centred(keys[2], (D, C), D ** -0.5, 0.125, ((0, 4), (1, 4))),
        "conv_taps": draw_conv_taps(jax.random.fold_in(keys[8], 71), part),
        "conv_bias": centred(keys[4], (C,), 0.5, 3.0, (), jnp.float32),
        "norm_gain": jnp.clip(1.0 + 0.18 * jax.random.normal(keys[5], (C,), jnp.float32), 0.1, 1.9),
        "norm_bias": centred(keys[6], (C,), 0.5, 3.0, (), jnp.float32),
        "out_weight": centred(keys[7], (C, D), C ** -0.5, 0.1875, ((0, 4), (1, 4))),
    }


epsilon = 1e-05

def one_sequence(rows, value_weight, gate_weight, conv_taps, conv_bias, norm_gain, norm_bias, out_weight):
    values = jnp.dot(rows, value_weight, preferred_element_type=jnp.float32).astype(jnp.bfloat16)
    gates = jnp.dot(rows, gate_weight, preferred_element_type=jnp.float32).astype(jnp.bfloat16)
    gated_rows = (values.astype(jnp.float32) * jax.nn.sigmoid(gates.astype(jnp.float32))).astype(jnp.bfloat16)
    padded = jnp.pad(gated_rows.astype(jnp.float32), ((KW - 1, 0), (0, 0)))
    length = rows.shape[0]
    conv_sum = jnp.zeros((length, C), jnp.float32) + conv_bias[None, :]
    for tap_index in range(KW):
        conv_sum = conv_sum + conv_taps[tap_index][None, :] * padded[tap_index:tap_index + length]
    mean_row = lax.optimization_barrier(jnp.mean(conv_sum, axis=-1, keepdims=True))
    centered = conv_sum - mean_row
    spread = lax.optimization_barrier(jnp.mean(centered * centered, axis=-1, keepdims=True))
    normed = centered * lax.rsqrt(spread + epsilon) * norm_gain[None, :] + norm_bias[None, :]
    swished = jax.nn.silu(normed).astype(jnp.bfloat16)
    return jnp.dot(swished, out_weight, preferred_element_type=jnp.float32).astype(jnp.bfloat16)

def reference(activations, value_weight, gate_weight, conv_taps, conv_bias, norm_gain, norm_bias, out_weight):

    def single(rows):
        return one_sequence(rows, value_weight, gate_weight, conv_taps, conv_bias, norm_gain, norm_bias, out_weight)
    return lax.map(single, activations)
```

```python
import functools

import jax
import jax.numpy as jnp
from jax import lax
from jax.experimental import pallas as pl
from jax.experimental.pallas import tpu as pltpu
from jax.sharding import PartitionSpec as P

epsilon = 1e-05
MESH = pl.DeviceIdType.MESH
LANES = 128


def kernel(
    cfg, x_ref, v_ref, g_ref, o_ref, taps_ref, bias_ref, gain_ref, shift_ref, out_ref,
    ext, w1, w2, acc, glu, conv, sw, outv, local_sem, halo_sem, send_sem, recv_w, recv_o,
):
    n, nd, T, H, KB, CB, OB, OC, KW, C = (cfg[k] for k in ("n", "nd", "T", "H", "KB", "CB", "OB", "OC", "KW", "C"))
    NW, NO = cfg["NW"], cfg["NO"]
    nx = nd // 2
    SUB = (NW, NO)
    y, z, d = lax.axis_index("grp"), lax.axis_index("sp"), lax.axis_index("dp")
    x, c = d // 2, d % 2
    has_down, has_up = z > 0, z < n - 1
    down, up = (y, jnp.maximum(z - 1, 0), d), (y, jnp.minimum(z + 1, n - 1), d)
    sibling = (y, z, x * 2 + 1 - c)
    across = (1 - y, z, d)
    columns = [lax.rem(x + dx, nx) * 2 + c for dx in range(1, nx)]

    barrier = pltpu.get_barrier_semaphore()

    def hello(target):
        pl.semaphore_signal(barrier, inc=1, device_id=target, device_id_type=MESH)

    own = [
        pltpu.make_async_copy(v_ref, w1.at[d, pl.ds(pl.multiple_of(z * KB, KB), KB), pl.ds(0, CB)], local_sem.at[0]),
        pltpu.make_async_copy(g_ref, w1.at[d, pl.ds(pl.multiple_of(z * KB, KB), KB), pl.ds(CB, CB)], local_sem.at[1]),
        pltpu.make_async_copy(o_ref, w2.at[d, pl.ds(pl.multiple_of(z * OB, OB), OB), :], local_sem.at[2]),
    ]
    rows = [
        pltpu.make_async_copy(x_ref.at[0, :, pl.ds(k * KB, KB)], ext.at[k, pl.ds(H, T), :], local_sem.at[3 + k])
        for k in range(n)
    ]
    for copy in own + rows:
        copy.start()
    pl.when(has_down)(lambda: hello(down))
    pl.when(has_up)(lambda: hello(up))
    hello(sibling)
    hello(across)
    for other in columns:
        hello((y, z, other))
    pl.semaphore_wait(barrier, nx + 1 + has_down.astype(jnp.int32) + has_up.astype(jnp.int32))

    def unit(kind, zz, dd, u):
        if kind == 0:
            size = KB // NW
            return w1.at[dd, pl.ds(pl.multiple_of(zz * KB + u * size, size), size), :]
        size = OB // NO
        return w2.at[dd, pl.ds(pl.multiple_of(zz * OB + u * size, size), size), :]

    def copy_of(kind, zz, dd, u, target):
        ref = unit(kind, zz, dd, u)
        return pltpu.make_async_remote_copy(
            src_ref=ref, dst_ref=ref, send_sem=send_sem.at[kind],
            recv_sem=(recv_w, recv_o)[kind].at[zz, dd, u], device_id=target, device_id_type=MESH,
        )

    def arrive(kind, zz, dd, u, drain):
        if not drain:
            copy_of(kind, zz, dd, u, sibling).wait_recv()

    def send(kind, zz, dd, u, target, drain):
        copy = copy_of(kind, zz, dd, u, target)
        copy.wait_send() if drain else copy.start()

    def both_ways(kind, e, body):
        sub = SUB[kind]
        r, u = e // sub, e % sub
        for sgn in (1, -1):
            zz = z + sgn * r
            valid = (zz >= 0) & (zz < n) & (r >= 0) & (r < n) & (e >= 0)
            if sgn == -1:
                valid = valid & (r > 0)
            pl.when(valid)(functools.partial(body, zz, r, u, sgn))

    def event_z(kind, e, drain=False):
        def body(zz, r, u, sgn):
            pl.when(r > 0)(lambda: arrive(kind, zz, d, u, drain))
            to_down = has_down if sgn == 1 else has_down & (r == 0)
            to_up = has_up & (r == 0) if sgn == 1 else has_up
            pl.when(to_down)(lambda: send(kind, zz, d, u, down, drain))
            pl.when(to_up)(lambda: send(kind, zz, d, u, up, drain))

            @pl.when(u % 2 == y)
            def _():
                for other in columns:
                    send(kind, zz, d, u, (y, z, other), drain)

            send(kind, zz, d, u, sibling, drain)

        both_ways(kind, e, body)

    def event_x(kind, e, drain=False):
        def body(zz, r, u, sgn):
            @pl.when(u % 2 == y)
            def _():
                for other in columns:
                    arrive(kind, zz, other, u, drain)
                    send(kind, zz, other, u, across, drain)
                    send(kind, zz, other, u, sibling, drain)

        both_ways(kind, e, body)

    def event_y(kind, e, drain=False):
        def body(zz, r, u, sgn):
            @pl.when(u % 2 != y)
            def _():
                for other in columns:
                    arrive(kind, zz, other, u, drain)
                    send(kind, zz, other, u, sibling, drain)

        both_ways(kind, e, body)

    def event_sibling(kind, e):
        def body(zz, r, u, sgn):
            for xx in range(nx):
                arrive(kind, zz, xx * 2 + 1 - c, u, False)

        both_ways(kind, e, body)

    def project(e):
        def body(zz, r, u, sgn):
            @pl.when(u == NW - 1)
            def _():
                def column(dd, _):
                    block = w1[dd, pl.ds(pl.multiple_of(zz * KB, KB), KB), :]
                    acc[dd] += jnp.dot(ext[zz], block, preferred_element_type=jnp.float32)
                    return 0

                lax.fori_loop(0, nd, column, 0)

        both_ways(0, e, body)

    halo = pltpu.make_async_remote_copy(
        src_ref=ext.at[:, pl.ds(T, H), :],
        dst_ref=ext.at[:, pl.ds(0, H), :],
        send_sem=halo_sem.at[0], recv_sem=halo_sem.at[1], device_id=up, device_id_type=MESH,
    )
    own[0].wait()
    own[1].wait()

    def first(e, _):
        event_z(0, e)
        return 0

    lax.fori_loop(0, NW, first, 0)
    for copy in rows:
        copy.wait()
    pl.when(has_up)(lambda: halo.start())
    own[2].wait()

    @pl.when(z == 0)
    def _():
        ext[:, 0:H, :] = jnp.zeros((n, H, KB), ext.dtype)

    def clear(dd, _):
        acc[dd] = jnp.zeros(acc.shape[1:], jnp.float32)
        return 0

    lax.fori_loop(0, nd, clear, 0)
    pl.when(has_down)(lambda: halo.wait_recv())

    def rest_of_step(e):
        event_x(0, e - cfg["LX"])
        event_y(0, e - cfg["LY"])
        event_sibling(0, e - cfg["LS"])
        project(e - cfg["LS"])

    def step(e, _):
        pl.when(e >= NW)(lambda: event_z(0, e))
        rest_of_step(e)
        return 0

    lax.fori_loop(0, n * NW, step, 0)

    def first_out(e, _):
        event_z(1, e)
        return 0

    lax.fori_loop(0, NO, first_out, 0)

    def last_steps(e, _):
        rest_of_step(e)
        return 0

    lax.fori_loop(n * NW, n * NW + cfg["LS"], last_steps, 0)

    GR = H
    per = CB // LANES

    def gate(i, _):
        at = pl.ds(pl.multiple_of(i * GR, GR), GR)
        for dd in range(nd):
            gated = acc[dd, at, 0:CB] * jax.nn.sigmoid(acc[dd, at, CB : 2 * CB])
            for p in range(per):
                glu[dd * per + p, at, :] = gated[:, p * LANES : (p + 1) * LANES]
        return 0

    lax.fori_loop(0, (T + H) // GR, gate, 0)

    R = cfg["R"]
    tiles = C // LANES
    offset = H - (KW - 1)
    reach = (offset + KW - 1) // 8 * 8

    def rows_of(i):
        base = pl.multiple_of(i * R, R)

        def channel(ct, total):
            lanes = pl.ds(pl.multiple_of(ct * LANES, LANES), LANES)
            block = glu[ct, pl.ds(base, R + H), :]
            block = jnp.concatenate([block, jnp.zeros((8, LANES), jnp.float32)], axis=0)
            value = jnp.broadcast_to(bias_ref[:, lanes], (R, LANES))
            for b in range(8):
                part = None
                for q in range(b, offset + KW, 8):
                    if q < offset:
                        continue
                    start = q - b
                    term = taps_ref[pl.ds(q - offset, 1), lanes] * block[start : start + R + 8]
                    part = term if part is None else part + term
                if part is not None:
                    value = value + part[b : b + R]
            conv[ct] = value
            return total + value

        total = lax.fori_loop(0, tiles, channel, jnp.zeros((R, LANES), jnp.float32))
        mean = jnp.sum(total, axis=-1, keepdims=True) * (1.0 / C)
        square = jnp.zeros((R, LANES), jnp.float32)
        for ct in range(tiles):
            centred = conv[ct] - mean
            square = square + centred * centred
        scale = lax.rsqrt(jnp.sum(square, axis=-1, keepdims=True) * (1.0 / C) + epsilon)
        for ct in range(tiles):
            lanes = slice(ct * LANES, (ct + 1) * LANES)
            normed = (conv[ct] - mean) * scale * gain_ref[:, lanes] + shift_ref[:, lanes]
            sw[pl.ds(base, R), lanes] = (normed * jax.nn.sigmoid(normed)).astype(sw.dtype)

    def out_step(e):
        pl.when(e >= NO)(lambda: event_z(1, e))
        event_x(1, e - 1)
        event_y(1, e - 2)
        event_sibling(1, e - 3)

    row_tiles = T // R
    out_steps = n * NO + 3

    def mixed(i, _):
        pl.when(i < row_tiles)(lambda: rows_of(i))
        pl.when(i < out_steps)(lambda: out_step(i))
        return 0

    lax.fori_loop(0, max(row_tiles, out_steps), mixed, 0)

    for dd in range(nd):
        outv[dd] = jnp.dot(sw[...], w2[dd], preferred_element_type=jnp.float32).astype(outv.dtype)
        pltpu.make_async_copy(outv.at[dd], out_ref.at[0, :, pl.ds(dd * OC, OC)], local_sem.at[dd]).start()

    pl.when(has_up)(lambda: halo.wait_send())
    for kind in (0, 1):
        def drain(e, _, kind=kind):
            event_z(kind, e, True)
            event_x(kind, e, True)
            event_y(kind, e, True)
            return 0

        lax.fori_loop(0, n * SUB[kind], drain, 0)
    for dd in range(nd):
        pltpu.make_async_copy(outv.at[dd], out_ref.at[0, :, pl.ds(dd * OC, OC)], local_sem.at[dd]).wait()


def local(activations, value_weight, gate_weight, conv_taps, conv_bias, norm_gain, norm_bias, out_weight):
    n, nd = lax.axis_size("sp"), lax.axis_size("dp")
    _, T, D = activations.shape
    KB, CB = value_weight.shape
    OB, OC = out_weight.shape
    KW, C = conv_taps.shape
    H = -(-(KW - 1) // 16) * 16
    NW = max(2, min(4, KB // 64))
    NO = 2
    cfg = dict(n=n, nd=nd, T=T, H=H, KB=KB, CB=CB, OB=OB, OC=OC, KW=KW, C=C, NW=NW, NO=NO, R=64, LX=2, LY=4, LS=5)
    anywhere = pl.BlockSpec(memory_space=pl.ANY)
    vmem = pl.BlockSpec(memory_space=pltpu.VMEM)
    bf16, f32 = jnp.bfloat16, jnp.float32
    return pl.pallas_call(
        functools.partial(kernel, cfg),
        out_shape=jax.ShapeDtypeStruct((1, T, D), bf16),
        in_specs=[anywhere] * 4 + [vmem] * 4,
        out_specs=anywhere,
        scratch_shapes=[
            pltpu.VMEM((n, T + H, KB), bf16),
            pltpu.VMEM((nd, n * KB, 2 * CB), bf16),
            pltpu.VMEM((nd, n * OB, OC), bf16),
            pltpu.VMEM((nd, T + H, 2 * CB), f32),
            pltpu.VMEM((C // LANES, T + H, LANES), f32),
            pltpu.VMEM((C // LANES, 64, LANES), f32),
            pltpu.VMEM((T, C), bf16),
            pltpu.VMEM((nd, T, OC), bf16),
            pltpu.SemaphoreType.DMA((max(nd, 3 + n),)),
            pltpu.SemaphoreType.DMA((2,)),
            pltpu.SemaphoreType.DMA((2,)),
            pltpu.SemaphoreType.DMA((n, nd, NW)),
            pltpu.SemaphoreType.DMA((n, nd, NO)),
        ],
        compiler_params=pltpu.CompilerParams(collective_id=0, has_side_effects=True, vmem_limit_bytes=56 * 2**20),
    )(
        activations, value_weight, gate_weight, out_weight,
        conv_taps, conv_bias[None], norm_gain[None], norm_bias[None],
    )


def solution(mesh):
    in_specs = (P(("grp", "dp"), "sp", None), P("sp", "dp"), P("sp", "dp"), P(), P(), P(), P(), P("sp", "dp"))
    out_specs = P(("grp", "dp"), "sp", None)
    return jax.shard_map(local, mesh=mesh, in_specs=in_specs, out_specs=out_specs, check_vma=False)
```

```python
import functools

import jax
import jax.numpy as jnp
from jax import lax
from jax.experimental import pallas as pl
from jax.experimental.pallas import tpu as pltpu
from jax.sharding import PartitionSpec as P

epsilon = 1e-05
MESH = pl.DeviceIdType.MESH
LANES = 128


def kernel(
    cfg, x_ref, v_ref, g_ref, o_ref, taps_ref, bias_ref, gain_ref, shift_ref, out_ref,
    ext, w1, w2, acc, glu, conv, sw, outv, local_sem, halo_sem, send_sem, recv_w, recv_o,
):
    n, nd, T, H, KB, CB, OB, OC, KW, C = (cfg[k] for k in ("n", "nd", "T", "H", "KB", "CB", "OB", "OC", "KW", "C"))
    NW, NO = cfg["NW"], cfg["NO"]
    nx = nd // 2
    SUB = (NW, NO)
    GROUP = (max(1, NW // 2), max(1, NO // 2))
    y, z, d = lax.axis_index("grp"), lax.axis_index("sp"), lax.axis_index("dp")
    x, c = d // 2, d % 2
    has_down, has_up = z > 0, z < n - 1
    down, up = (y, jnp.maximum(z - 1, 0), d), (y, jnp.minimum(z + 1, n - 1), d)
    sibling = (y, z, x * 2 + 1 - c)
    across = (1 - y, z, d)
    columns = [lax.rem(x + dx, nx) * 2 + c for dx in range(1, nx)]

    barrier = pltpu.get_barrier_semaphore()

    def hello(target):
        pl.semaphore_signal(barrier, inc=1, device_id=target, device_id_type=MESH)

    own = [
        pltpu.make_async_copy(v_ref, w1.at[d, pl.ds(pl.multiple_of(z * KB, KB), KB), pl.ds(0, CB)], local_sem.at[0]),
        pltpu.make_async_copy(g_ref, w1.at[d, pl.ds(pl.multiple_of(z * KB, KB), KB), pl.ds(CB, CB)], local_sem.at[1]),
        pltpu.make_async_copy(o_ref, w2.at[d, pl.ds(pl.multiple_of(z * OB, OB), OB), :], local_sem.at[2]),
    ]
    rows = [
        pltpu.make_async_copy(x_ref.at[0, :, pl.ds(k * KB, KB)], ext.at[k, pl.ds(H, T), :], local_sem.at[3 + k])
        for k in range(n)
    ]
    for copy in own + rows:
        copy.start()
    pl.when(has_down)(lambda: hello(down))
    pl.when(has_up)(lambda: hello(up))
    hello(sibling)
    hello(across)
    for other in columns:
        hello((y, z, other))
    pl.semaphore_wait(barrier, nx + 1 + has_down.astype(jnp.int32) + has_up.astype(jnp.int32))

    def unit(kind, zz, dd, u):
        if kind == 0:
            size = KB // NW
            return w1.at[dd, pl.ds(pl.multiple_of(zz * KB + u * size, size), size), :]
        size = OB // NO
        return w2.at[dd, pl.ds(pl.multiple_of(zz * OB + u * size, size), size), :]

    def copy_of(kind, zz, dd, u, target):
        ref = unit(kind, zz, dd, u)
        return pltpu.make_async_remote_copy(
            src_ref=ref, dst_ref=ref, send_sem=send_sem.at[kind],
            recv_sem=(recv_w, recv_o)[kind].at[zz, dd, u], device_id=target, device_id_type=MESH,
        )

    def arrive(kind, zz, dd, u, drain):
        if not drain:
            copy_of(kind, zz, dd, u, sibling).wait_recv()

    def send(kind, zz, dd, u, target, drain):
        copy = copy_of(kind, zz, dd, u, target)
        copy.wait_send() if drain else copy.start()

    def both_ways(kind, e, body):
        sub = SUB[kind]
        r, u = e // sub, e % sub
        for sgn in (1, -1):
            zz = z + sgn * r
            valid = (zz >= 0) & (zz < n) & (r >= 0) & (r < n) & (e >= 0)
            if sgn == -1:
                valid = valid & (r > 0)
            pl.when(valid)(functools.partial(body, zz, r, u, sgn))

    at_end = (z == 0) | (z == n - 1)

    def skipped(kind, r, u, plane):
        return (u % 2 != plane) & ((u // 2 % 2 == 0) | (kind == 0)) & (r < n - 1 if kind == 0 else r < n - 2)

    def both_planes(kind, r):
        return r >= (n if kind == 0 else n - 2)

    def direct(kind, r, u):
        return (u % 2 == y) | both_planes(kind, r)

    def event_z(kind, e, drain=False):
        def body(zz, r, u, sgn):
            detour = at_end & (r > 0)

            @pl.when(jnp.logical_not(detour & skipped(kind, r, u, y)))
            def _():
                pl.when(r > 0)(lambda: arrive(kind, zz, d, u, drain))
                to_down = has_down if sgn == 1 else has_down & (r == 0)
                to_up = has_up & (r == 0) if sgn == 1 else has_up
                to_down = to_down & jnp.logical_not((z == 1) & skipped(kind, r + 1, u, y))
                to_up = to_up & jnp.logical_not((z == n - 2) & skipped(kind, r + 1, u, y))
                pl.when(to_down)(lambda: send(kind, zz, d, u, down, drain))
                pl.when(to_up)(lambda: send(kind, zz, d, u, up, drain))
                pl.when(detour & skipped(kind, r, u, 1 - y))(lambda: send(kind, zz, d, u, across, drain))

                @pl.when(direct(kind, r, u))
                def _():
                    for other in columns:
                        send(kind, zz, d, u, (y, z, other), drain)

        both_ways(kind, e, body)

    def event_x(kind, e, drain=False):
        def body(zz, r, u, sgn):
            @pl.when(direct(kind, r, u))
            def _():
                for other in columns:
                    arrive(kind, zz, other, u, drain)
                    pl.when(jnp.logical_not(both_planes(kind, r)))(
                        functools.partial(send, kind, zz, other, u, across, drain)
                    )

        both_ways(kind, e, body)

    def event_y(kind, e, drain=False):
        def body(zz, r, u, sgn):
            @pl.when(jnp.logical_not(direct(kind, r, u)))
            def _():
                for other in columns:
                    arrive(kind, zz, other, u, drain)

            @pl.when(at_end & (r > 0) & skipped(kind, r, u, y))
            def _():
                arrive(kind, zz, d, u, drain)

        both_ways(kind, e, body)

    def group_of(kind, zz, dd, u):
        size = (KB // NW, OB // NO)[kind]
        many = GROUP[kind]
        first_row = zz * size * SUB[kind] + (u - many + 1) * size
        ref = (w1, w2)[kind].at[dd, pl.ds(pl.multiple_of(first_row, size * many), size * many), :]
        return pltpu.make_async_remote_copy(
            src_ref=ref, dst_ref=ref, send_sem=send_sem.at[kind],
            recv_sem=(recv_w, recv_o)[kind].at[zz, dd, u], device_id=sibling, device_id_type=MESH,
        )

    def event_hand(kind, e, drain=False):
        def body(zz, r, u, sgn):
            @pl.when(u % GROUP[kind] == GROUP[kind] - 1)
            def _():
                for xx in range(nx):
                    copy = group_of(kind, zz, xx * 2 + c, u)
                    copy.wait_send() if drain else copy.start()

        both_ways(kind, e, body)

    def event_sibling(kind, e):
        def body(zz, r, u, sgn):
            @pl.when(u % GROUP[kind] == GROUP[kind] - 1)
            def _():
                for xx in range(nx):
                    group_of(kind, zz, xx * 2 + 1 - c, u).wait_recv()

        both_ways(kind, e, body)

    def project(e):
        def body(zz, r, u, sgn):
            per_step = -(-nd // NW)

            @pl.when(u * per_step < nd)
            def _():
                def column(k, _):
                    dd = u * per_step + k
                    block = w1[dd, pl.ds(pl.multiple_of(zz * KB, KB), KB), :]
                    acc[dd] += jnp.dot(ext[zz], block, preferred_element_type=jnp.float32)
                    return 0

                lax.fori_loop(0, per_step, column, 0)

        both_ways(0, e, body)

    halo = pltpu.make_async_remote_copy(
        src_ref=ext.at[:, pl.ds(T, H), :],
        dst_ref=ext.at[:, pl.ds(0, H), :],
        send_sem=halo_sem.at[0], recv_sem=halo_sem.at[1], device_id=up, device_id_type=MESH,
    )
    own[0].wait()
    own[1].wait()

    def first(e, _):
        event_z(0, e)
        return 0

    lax.fori_loop(0, NW, first, 0)
    for copy in rows:
        copy.wait()
    pl.when(has_up)(lambda: halo.start())
    own[2].wait()

    @pl.when(z == 0)
    def _():
        ext[:, 0:H, :] = jnp.zeros((n, H, KB), ext.dtype)

    def clear(dd, _):
        acc[dd] = jnp.zeros(acc.shape[1:], jnp.float32)
        return 0

    lax.fori_loop(0, nd, clear, 0)
    pl.when(has_down)(lambda: halo.wait_recv())

    EW, EO = n * NW, n * NO
    LX, LY, LS = cfg["LX"], cfg["LY"], cfg["LS"]
    MX, MY, MS = cfg["MX"], cfg["MY"], cfg["MS"]
    EARLY = cfg["EARLY"] * NW

    def weights_rest(e):
        event_x(0, e - LX)
        event_y(0, e - LY)
        event_hand(0, e - LY)
        event_sibling(0, e - LS)
        project(e - LS - NW + 1)

    def out_step(e):
        pl.when(e >= NO)(lambda: event_z(1, e))
        event_x(1, e - MX)
        event_y(1, e - MY)
        event_hand(1, e - MY)
        event_sibling(1, e - MS)

    def weights_step(e, _):
        pl.when((e >= EARLY) & (e < EARLY + NO))(lambda: event_z(1, e - EARLY))
        pl.when(e >= NW)(lambda: event_z(0, e))
        weights_rest(e)
        return 0

    lax.fori_loop(0, EW, weights_step, 0)
    tail = LS + NW - 1
    ahead = max(0, n - 2) * NO

    def tail_step(t, _):
        pl.when((t % 2 == 1) & (t // 2 < ahead))(lambda: out_step(NO + t // 2))
        weights_rest(EW + t)
        return 0

    lax.fori_loop(0, tail, tail_step, 0)
    done = NO + min(ahead, tail // 2)

    GR = H
    per = CB // LANES

    def gate(i, _):
        at = pl.ds(pl.multiple_of(i * GR, GR), GR)
        for dd in range(nd):
            gated = acc[dd, at, 0:CB] * jax.nn.sigmoid(acc[dd, at, CB : 2 * CB])
            for p in range(per):
                glu[dd * per + p, at, :] = gated[:, p * LANES : (p + 1) * LANES]
        return 0

    lax.fori_loop(0, (T + H) // GR, gate, 0)

    R = cfg["R"]
    tiles = C // LANES
    offset = H - (KW - 1)
    reach = (offset + KW - 1) // 8 * 8

    def rows_of(i):
        base = pl.multiple_of(i * R, R)

        def channel(ct, total):
            lanes = pl.ds(pl.multiple_of(ct * LANES, LANES), LANES)
            block = glu[ct, pl.ds(base, R + H), :]
            block = jnp.concatenate([block, jnp.zeros((8, LANES), jnp.float32)], axis=0)
            value = jnp.broadcast_to(bias_ref[:, lanes], (R, LANES))
            for b in range(8):
                part = None
                for q in range(b, offset + KW, 8):
                    if q < offset:
                        continue
                    start = q - b
                    term = taps_ref[pl.ds(q - offset, 1), lanes] * block[start : start + R + 8]
                    part = term if part is None else part + term
                if part is not None:
                    value = value + part[b : b + R]
            conv[ct] = value
            return total + value

        total = lax.fori_loop(0, tiles, channel, jnp.zeros((R, LANES), jnp.float32))
        mean = jnp.sum(total, axis=-1, keepdims=True) * (1.0 / C)
        square = jnp.zeros((R, LANES), jnp.float32)
        for ct in range(tiles):
            centred = conv[ct] - mean
            square = square + centred * centred
        scale = lax.rsqrt(jnp.sum(square, axis=-1, keepdims=True) * (1.0 / C) + epsilon)
        for ct in range(tiles):
            lanes = slice(ct * LANES, (ct + 1) * LANES)
            normed = (conv[ct] - mean) * scale * gain_ref[:, lanes] + shift_ref[:, lanes]
            sw[pl.ds(base, R), lanes] = (normed * jax.nn.sigmoid(normed)).astype(sw.dtype)

    def drain(kind, e, _):
        event_z(kind, e, True)
        event_x(kind, e, True)
        event_y(kind, e, True)
        event_hand(kind, e, True)
        return 0

    row_tiles = T // R
    drained = -(-EW // row_tiles)
    each = -(-(EO + MS - done) // row_tiles)

    def mixed(i, _):
        rows_of(i)

        def one(k, _):
            out_step(done + i * each + k)
            return 0

        lax.fori_loop(0, each, one, 0)
        lax.fori_loop(i * drained, (i + 1) * drained, functools.partial(drain, 0), 0)
        return 0

    lax.fori_loop(0, row_tiles, mixed, 0)

    for dd in range(nd):
        outv[dd] = jnp.dot(sw[...], w2[dd], preferred_element_type=jnp.float32).astype(outv.dtype)
        pltpu.make_async_copy(outv.at[dd], out_ref.at[0, :, pl.ds(dd * OC, OC)], local_sem.at[dd]).start()

    pl.when(has_up)(lambda: halo.wait_send())
    lax.fori_loop(0, EO, functools.partial(drain, 1), 0)
    for dd in range(nd):
        pltpu.make_async_copy(outv.at[dd], out_ref.at[0, :, pl.ds(dd * OC, OC)], local_sem.at[dd]).wait()


def local(activations, value_weight, gate_weight, conv_taps, conv_bias, norm_gain, norm_bias, out_weight):
    n, nd = lax.axis_size("sp"), lax.axis_size("dp")
    _, T, D = activations.shape
    KB, CB = value_weight.shape
    OB, OC = out_weight.shape
    KW, C = conv_taps.shape
    H = -(-(KW - 1) // 16) * 16
    NW = max(2, min(8, KB // 64))
    NO = max(2, min(4, OB // 64))
    cfg = dict(n=n, nd=nd, T=T, H=H, KB=KB, CB=CB, OB=OB, OC=OC, KW=KW, C=C, NW=NW, NO=NO, R=64, LX=4, LY=10, LS=12, MX=4, MY=7, MS=9, EARLY=min(3, n - 1))
    anywhere = pl.BlockSpec(memory_space=pl.ANY)
    vmem = pl.BlockSpec(memory_space=pltpu.VMEM)
    bf16, f32 = jnp.bfloat16, jnp.float32
    return pl.pallas_call(
        functools.partial(kernel, cfg),
        out_shape=jax.ShapeDtypeStruct((1, T, D), bf16),
        in_specs=[anywhere] * 4 + [vmem] * 4,
        out_specs=anywhere,
        scratch_shapes=[
            pltpu.VMEM((n, T + H, KB), bf16),
            pltpu.VMEM((nd, n * KB, 2 * CB), bf16),
            pltpu.VMEM((nd, n * OB, OC), bf16),
            pltpu.VMEM((nd, T + H, 2 * CB), f32),
            pltpu.VMEM((C // LANES, T + H, LANES), f32),
            pltpu.VMEM((C // LANES, 64, LANES), f32),
            pltpu.VMEM((T, C), bf16),
            pltpu.VMEM((nd, T, OC), bf16),
            pltpu.SemaphoreType.DMA((max(nd, 3 + n),)),
            pltpu.SemaphoreType.DMA((2,)),
            pltpu.SemaphoreType.DMA((2,)),
            pltpu.SemaphoreType.DMA((n, nd, NW)),
            pltpu.SemaphoreType.DMA((n, nd, NO)),
        ],
        compiler_params=pltpu.CompilerParams(collective_id=0, has_side_effects=True, vmem_limit_bytes=56 * 2**20),
    )(
        activations, value_weight, gate_weight, out_weight,
        conv_taps, conv_bias[None], norm_gain[None], norm_bias[None],
    )


def solution(mesh):
    in_specs = (P(("grp", "dp"), "sp", None), P("sp", "dp"), P("sp", "dp"), P(), P(), P(), P(), P("sp", "dp"))
    out_specs = P(("grp", "dp"), "sp", None)
    return jax.shard_map(local, mesh=mesh, in_specs=in_specs, out_specs=out_specs, check_vma=False)
```
